32 devices in a mesh: grp: 2 (over x), tp: 4 (over z), dp: 4 (over y, core).
Axes of the slice: x: 2, y: 2, z: 4, core: 2. Of those that a mesh axis runs over, the one named last changes fastest.
Arguments:
- tokens: bfloat16 [8, 4, 4096], P(('grp', 'tp'), None, 'dp'), parts along dimension 0, may hold values from -6 to 6
- lengths: int32 [8], P('grp'), parts along dimension 0, may hold values from 1 to 4, 8 in all
- norm_gain: float32 [2, 4096], P(None, 'dp'), may hold values from 0.1 to 1.9
- input_weight: bfloat16 [2, 4096, 8192], P(None, 'dp', 'tp'), may hold values from -0.09375 to 0.09375
- gate_weight: bfloat16 [2, 4096, 8192], P(None, 'dp', 'tp'), may hold values from -0.09375 to 0.09375
- decay_rate: float32 [2, 512, 64], P(None, 'tp'), may hold values from 0.05 to 2
- frequency: float32 [2, 512, 64], P(None, 'tp'), may hold values from 0 to 4
- log_step: float32 [2, 512], P(None, 'tp'), may hold values from -2.3 to 0
- input_map: bfloat16 [2, 512, 16, 128], P(None, 'tp'), may hold values from -1 to 1
- readout_map: bfloat16 [2, 512, 16, 128], P(None, 'tp'), may hold values from -0.5 to 0.5
- skip_weight: bfloat16 [2, 8192], P(None, 'tp'), may hold values from -4 to 4
- out_weight: bfloat16 [2, 8192, 4096], P(None, 'tp', 'dp'), may hold values from -0.0625 to 0.0625
- state: float32 [2, 8, 512, 128], P(None, ('grp', 'dp'), 'tp'), parts along dimension 1, may hold values from -5 to 5
Outputs:
- mixed: bfloat16 [8, 4, 4096], P(('grp', 'tp'), None, 'dp'), parts along dimension 0
- new_state: float32 [2, 8, 512, 128], P(None, ('grp', 'dp'), 'tp'), parts along dimension 1
The draws below stay inside these ranges and needn't reach their ends.
There are 2 independent parts, one for each index of `grp`. The reference program is written for one: setup_inputs(seed, part) draws one part's arguments, and reference() takes and returns one part's arrays. A program takes and returns all parts, laid end to end along the dimension named above; an argument that names none is the same for every part. Nothing has to cross between parts.
Inputs may be any that keep to these rules, and one draw needn't show every extreme that they name: `lengths`: the number of live new positions of each sequence; positions beyond it take no part.
All inputs are finite; a program needn't handle non-finite values.
Results may differ from the reference program's by a relative error of at most 0.023.
Values may be sent and summed in bfloat16 or wider, within the bound.
A program may use at most 64 MiB of HBM per device.

```python
import math
import jax
import jax.numpy as jnp
import numpy as np
from jax import lax

D = 4096
E = 8192
S5_IN = 16
P_SIZE = 64
NEW = 4
LAYERS = 2
GROUPS = 512
SEQS = 4


def shard_levels(stream_key, extent, shards, low, high):
    def one(axis_at, parts):
        heights = jax.random.uniform(jax.random.fold_in(jax.random.fold_in(stream_key, 6), axis_at), (parts,), jnp.float32, low / len(shards), high / len(shards))
        return jnp.repeat(jnp.exp(heights), extent[axis_at] // parts).reshape((-1,) + (1,) * (len(extent) - axis_at - 1))

    factor_of = one(*shards[0])
    for cut in shards[1:]:
        factor_of = factor_of * one(*cut)
    return factor_of


def profile(count, total, limit, slope):
    portions = [(1 << 20) // math.isqrt(grade ** slope) + 1 for grade in range(2, count + 1)]
    rest, holding = total - limit - (count - 1), [1] * (count - 1)
    while rest > 0:
        movable = [i for i in range(count - 1) if holding[i] < limit]
        pool, budget = sum([portions[i] for i in movable]), rest
        for i in movable:
            extra = min(limit - holding[i], max(1, budget * portions[i] // pool), rest)
            holding[i] = holding[i] + extra
            rest = rest - extra
    return np.array([limit] + holding)


def ragged(own_key, count, total, bound, lean):
    if count == 2:
        one = jax.random.randint(own_key, (), max(1, total - bound), min(bound, total - 1) + 1)
        return jnp.stack([one, total - one])
    sizes = jnp.asarray(profile(count, total, bound, lean), jnp.int32)
    pairs = (count - 1) // 2
    source_of, receiver = sizes[1:1 + 2 * pairs:2], sizes[2:2 + 2 * pairs:2]
    slack = jnp.minimum(source_of - 1, bound - receiver)
    shifted = jax.random.randint(jax.random.fold_in(own_key, 1), (pairs,), 0, 1 << 20) % (slack + 1)
    sizes = sizes.at[1:1 + 2 * pairs:2].set(source_of - shifted).at[2:2 + 2 * pairs:2].set(receiver + shifted)
    return sizes[jax.random.permutation(jax.random.fold_in(own_key, 2), count)]


def gaussian(own_key, extent, width, limit, split=(), held_as=jnp.bfloat16):
    drawn = jax.random.normal(own_key, extent, jnp.float32) * width
    if len(split) > 0:
        drawn = shard_levels(own_key, extent, split, -0.22, 0.18) * drawn
    return jnp.clip(drawn, min=-limit, max=limit).astype(held_as)


def setup_inputs(seed: int = 0, part: int = 0) -> dict:
    splits = jax.random.split(jax.random.key(seed), 14)
    part_splits = jax.random.split(jax.random.fold_in(splits[13], part), 14)
    return {
        "tokens": gaussian(part_splits[0], (SEQS, NEW, D), 1.0, 6.0, ((0, 4), (2, 4))),
        "lengths": ragged(part_splits[1], SEQS, 2 * SEQS, NEW, 2).astype(jnp.int32),
        "norm_gain": jnp.clip(1.0 + 0.18 * jax.random.normal(splits[2], (LAYERS, D), jnp.float32), 0.1, 1.9),
        "input_weight": gaussian(splits[3], (LAYERS, D, E), D ** -0.5, 0.09375, ((1, 4), (2, 4))),
        "gate_weight": gaussian(splits[4], (LAYERS, D, E), D ** -0.5, 0.09375, ((1, 4), (2, 4))),
        "decay_rate": jnp.clip(jnp.exp(math.log(2.0) - 3.6888794 * jax.random.uniform(splits[5], (LAYERS, GROUPS, P_SIZE), jnp.float32) ** shard_levels(splits[5], (LAYERS, GROUPS, P_SIZE), ((1, 4),), -0.2, 0.2)), 0.05, 2.0),
        "frequency": jnp.clip(4.0 * jax.random.uniform(splits[6], (LAYERS, GROUPS, P_SIZE), jnp.float32) ** shard_levels(splits[6], (LAYERS, GROUPS, P_SIZE), ((1, 4),), -0.2, 0.2), 0.0, 4.0),
        "log_step": jnp.clip(-2.3 + 2.3 * jax.random.uniform(splits[7], (LAYERS, GROUPS), jnp.float32) ** shard_levels(splits[7], (LAYERS, GROUPS), ((1, 4),), -0.2, 0.2), -2.3, 0.0),
        "input_map": gaussian(splits[8], (LAYERS, GROUPS, S5_IN, 2 * P_SIZE), (2 * S5_IN) ** -0.5, 1.0, ((1, 4),)),
        "readout_map": gaussian(splits[9], (LAYERS, GROUPS, S5_IN, 2 * P_SIZE), (2 * P_SIZE) ** -0.5, 0.5, ((1, 4),)),
        "skip_weight": gaussian(splits[10], (LAYERS, E), 1.0, 4.0, ((1, 4),)),
        "out_weight": gaussian(splits[11], (LAYERS, E, D), E ** -0.5, 0.0625, ((1, 4), (2, 4))),
        "state": gaussian(part_splits[12], (LAYERS, SEQS, GROUPS, 2 * P_SIZE), 0.7, 5.0, ((1, 4), (2, 4)), jnp.float32),
    }


epsilon = 1e-06

def advance_state(drive_value, gate_value, carried, alive_mask, decay_rate, frequency, log_step, input_map, readout_map, skip_row):
    seq_count, new_count, inner_width = drive_value.shape
    group_count = inner_width // S5_IN
    state_half = carried.shape[-1] // 2
    step_size = jnp.exp(log_step)[:, None]
    magnitude = jnp.exp(-decay_rate * step_size)
    turn_angle = frequency * step_size
    decay_real = magnitude * jnp.cos(turn_angle)
    decay_imag = magnitude * jnp.sin(turn_angle)
    denominator = decay_rate * decay_rate + frequency * frequency
    coeff_real = (-(decay_real - 1.0) * decay_rate + decay_imag * frequency) / denominator
    coeff_imag = (-decay_imag * decay_rate - (decay_real - 1.0) * frequency) / denominator
    map_real = input_map[..., :state_half].astype(jnp.float32)
    map_imag = input_map[..., state_half:].astype(jnp.float32)
    coupled = jnp.concatenate([coeff_real[:, None, :] * map_real - coeff_imag[:, None, :] * map_imag, coeff_real[:, None, :] * map_imag + coeff_imag[:, None, :] * map_real], axis=-1)
    inputs = drive_value.astype(jnp.float32).reshape(seq_count, new_count, group_count, S5_IN)
    pushed = jnp.einsum('stgi,giq->stgq', inputs, coupled, precision=lax.Precision.HIGHEST)
    real_state = carried[..., :state_half]
    imag_state = carried[..., state_half:]
    history = []
    for position in range(new_count):
        keep = alive_mask[:, position][:, None, None] > 0.5
        next_real = decay_real * real_state - decay_imag * imag_state + pushed[:, position, :, :state_half]
        next_imag = decay_real * imag_state + decay_imag * real_state + pushed[:, position, :, state_half:]
        real_state = jnp.where(keep, next_real, real_state)
        imag_state = jnp.where(keep, next_imag, imag_state)
        history.append(jnp.concatenate([real_state, -imag_state], axis=-1))
    stacked = jnp.stack(history, axis=1)
    readout = jnp.einsum('stgq,giq->stgi', stacked, readout_map.astype(jnp.float32), precision=lax.Precision.HIGHEST)
    readout = readout.reshape(seq_count, new_count, inner_width)
    response = readout + skip_row.astype(jnp.float32) * inputs.reshape(seq_count, new_count, inner_width)
    branch = jax.nn.gelu(response) * jax.nn.silu(gate_value.astype(jnp.float32)) * alive_mask[:, :, None]
    return (jnp.concatenate([real_state, imag_state], axis=-1), branch.astype(jnp.bfloat16))

def reference(tokens, lengths, norm_gain, input_weight, gate_weight, decay_rate, frequency, log_step, input_map, readout_map, skip_weight, out_weight, state):
    seq_count, new_count, model_width = tokens.shape
    positions = lax.broadcasted_iota(jnp.int32, (seq_count, new_count), 1)
    alive_mask = (positions < lengths[:, None]).astype(jnp.float32)
    current = tokens
    states = []
    for layer_index in range(LAYERS):
        flattened = current.reshape(seq_count * new_count, model_width).astype(jnp.float32)
        inverse = lax.rsqrt(lax.optimization_barrier(jnp.mean(flattened * flattened, axis=1)) + epsilon)[:, None]
        scaled = (flattened * norm_gain[layer_index][None, :]).astype(jnp.bfloat16)
        drive_value = (inverse * jnp.dot(scaled, input_weight[layer_index], preferred_element_type=jnp.float32)).astype(jnp.bfloat16)
        gate_value = (inverse * jnp.dot(scaled, gate_weight[layer_index], preferred_element_type=jnp.float32)).astype(jnp.bfloat16)
        inner_width = drive_value.shape[1]
        next_state, branch = advance_state(drive_value.reshape(seq_count, new_count, inner_width), gate_value.reshape(seq_count, new_count, inner_width), state[layer_index], alive_mask, decay_rate[layer_index], frequency[layer_index], log_step[layer_index], input_map[layer_index], readout_map[layer_index], skip_weight[layer_index])
        states.append(next_state)
        projected = jnp.dot(branch.reshape(seq_count * new_count, inner_width), out_weight[layer_index], preferred_element_type=jnp.float32)
        current = (flattened + projected).astype(jnp.bfloat16).reshape(tokens.shape)
    return (current, jnp.stack(states))
```

```python
import functools

import jax
import jax.numpy as jnp
from jax import lax
from jax.experimental import pallas as pl
from jax.experimental.pallas import tpu as pltpu
from jax.sharding import PartitionSpec as P

D = 4096
S5_IN = 16
CHUNKS = 4
LANES = 128

epsilon = 1e-06
f32, bf16 = jnp.float32, jnp.bfloat16


def kernel(
    n_tp,
    n_dp,
    lengths,
    tokens,
    norm_gain,
    input_weight,
    gate_weight,
    decay_rate,
    frequency,
    log_step,
    input_map,
    readout_map,
    skip_weight,
    out_weight,
    state,
    mixed_out,
    state_out,
    v_gain,
    v_in,
    v_gate,
    v_decay,
    v_freq,
    v_step,
    v_imap,
    v_rmap,
    v_skip,
    v_out,
    v_state,
    v_mixed,
    x_recv,
    x_all,
    sq_send,
    sq_recv,
    part_send,
    part_recv,
    branch_all,
    b_rows,
    read_rows,
    tp_all,
    rs_send,
    rs_recv,
    coef,
    sem_small,
    sem_w,
    sem_out,
    sem_x,
    sem_sq,
    sem_part,
    sem_branch,
    sem_tp,
    sem_rs,
):
    layers, own_seqs, groups, state_width = state.shape
    block_rows, features = tokens.shape
    inner = input_weight.shape[2]
    width = inner // CHUNKS
    all_seqs = lengths.shape[0]
    new = block_rows * n_tp // all_seqs
    own_rows = own_seqs * new
    rows = all_seqs * new
    half = state_width // 2
    per_tile = LANES // S5_IN
    tiles = width // LANES
    tp_me = lax.axis_index("tp")
    dp_me = lax.axis_index("dp")

    def local(src, dst, sem):
        copy = pltpu.make_async_copy(src, dst, sem)
        copy.start()
        return copy

    small = [
        local(src, dst, sem_small.at[i])
        for i, (src, dst) in enumerate(
            (
                (tokens, x_recv.at[tp_me]),
                (norm_gain, v_gain),
                (decay_rate, v_decay),
                (frequency, v_freq),
                (log_step, v_step),
                (skip_weight, v_skip),
                (state, v_state),
            )
        )
    ]
    fetch = {}
    for l in range(layers):
        for n in range(CHUNKS):
            cols = pl.ds(n * width, width)
            fetch["in", l, n] = local(input_weight.at[l, :, cols], v_in.at[l, n], sem_w.at[l, n, 0])
            fetch["gate", l, n] = local(gate_weight.at[l, :, cols], v_gate.at[l, n], sem_w.at[l, n, 1])
        fetch["imap", l] = local(input_map.at[l], v_imap.at[l], sem_w.at[l, 0, 3])
        fetch["rmap", l] = local(readout_map.at[l], v_rmap.at[l], sem_w.at[l, 1, 3])
        for n in range(CHUNKS):
            cols = pl.ds(n * width, width)
            fetch["out", l, n] = local(out_weight.at[l, cols, :], v_out.at[l, n], sem_w.at[l, n, 2])

    barrier = pltpu.get_barrier_semaphore()
    tp_peers = [lax.rem(tp_me + k, n_tp) for k in range(1, n_tp)]
    dp_peers = [lax.rem(dp_me + k, n_dp) for k in range(1, n_dp)]
    for peer in tp_peers:
        pl.semaphore_signal(
            barrier, inc=1, device_id={"tp": peer}, device_id_type=pl.DeviceIdType.MESH
        )
    for peer in dp_peers:
        pl.semaphore_signal(
            barrier, inc=1, device_id={"dp": peer}, device_id_type=pl.DeviceIdType.MESH
        )
    pl.semaphore_wait(barrier, n_tp + n_dp - 2)

    sends = []

    def push(axis, peer, src, dst, sems):
        copy = pltpu.make_async_remote_copy(
            src_ref=src,
            dst_ref=dst,
            send_sem=sems.at[0],
            recv_sem=sems.at[1],
            device_id={axis: peer},
            device_id_type=pl.DeviceIdType.MESH,
        )
        copy.start()

    def settle(ref, sem):
        pltpu.make_async_copy(ref, ref, sem).wait()

    small[0].wait()
    for peer in tp_peers:
        push("tp", peer, x_recv.at[tp_me], x_recv.at[tp_me], sem_x)
    sends.append((x_recv.at[pl.ds(0, n_tp - 1)], sem_x.at[0]))

    for copy in small[1:]:
        copy.wait()
    for l in range(layers):
        step = jnp.exp(jnp.broadcast_to(v_step[l : l + 1, :], (LANES, groups)).T)[:, :half]
        rate = v_decay[l]
        freq = v_freq[l]
        magnitude = jnp.exp(-rate * step)
        angle = freq * step
        ar = magnitude * jnp.cos(angle)
        ai = magnitude * jnp.sin(angle)
        den = rate * rate + freq * freq
        cr = (-(ar - 1.0) * rate + ai * freq) / den
        ci = (-ai * rate - (ar - 1.0) * freq) / den
        for i, (low, high) in enumerate(((ar, ar), (-ai, ai), (cr, cr), (-ci, ci))):
            coef[l, i, :, 0:half] = low
            coef[l, i, :, half:] = high

    settle(x_recv.at[pl.ds(0, n_tp - 1)], sem_x.at[1])
    for j in range(n_tp):
        x_all[j * block_rows : (j + 1) * block_rows, :] = x_recv[j].astype(f32)
    x = x_all[...]

    lane = lax.broadcasted_iota(jnp.int32, (per_tile, LANES), 1)
    sub = lax.broadcasted_iota(jnp.int32, (per_tile, LANES), 0)
    own_group = (lane >= sub * S5_IN) & (lane < (sub + 1) * S5_IN)
    sign = jnp.where(
        lax.broadcasted_iota(jnp.int32, (1, state_width), 1) < half, jnp.float32(1), jnp.float32(-1)
    )
    lens = [lengths[dp_me * own_seqs + s] for s in range(own_seqs)]
    row_id = lax.broadcasted_iota(jnp.int32, (own_rows, 1), 0)
    alive = jnp.zeros((own_rows, 1), f32)
    for s in range(own_seqs):
        inside = (row_id >= s * new) & (row_id < s * new + lens[s])
        alive = jnp.where(inside, jnp.float32(1), alive)

    for l in range(layers):
        squares = jnp.sum(x * x, axis=1, keepdims=True)
        wide = jnp.broadcast_to(squares, (rows, LANES))
        for j in range(n_dp):
            sq_send[l, j] = wide[j * own_rows : (j + 1) * own_rows, :]
        for k, peer in enumerate(dp_peers):
            push("dp", peer, sq_send.at[l, peer], sq_recv.at[l, k], sem_sq.at[l])
        sends.append((sq_recv.at[l], sem_sq.at[l, 0]))
        scaled = (x * v_gain[l : l + 1, :]).astype(bf16)
        for n in range(CHUNKS):
            fetch["in", l, n].wait()
            drive_part = jnp.dot(scaled, v_in[l, n], preferred_element_type=f32)
            fetch["gate", l, n].wait()
            gate_part = jnp.dot(scaled, v_gate[l, n], preferred_element_type=f32)
            for j in range(n_dp):
                own = slice(j * own_rows, (j + 1) * own_rows)
                part_send[l, n, j, :, 0:width] = drive_part[own].astype(bf16)
                part_send[l, n, j, :, width:] = gate_part[own].astype(bf16)
            for k, peer in enumerate(dp_peers):
                push("dp", peer, part_send.at[l, n, peer], part_recv.at[l, n, k], sem_part.at[l, n])
            sends.append((part_recv.at[l, n], sem_part.at[l, n, 0]))

        fetch["imap", l].wait()
        fetch["rmap", l].wait()
        settle(sq_recv.at[l], sem_sq.at[l, 1])
        total = sq_send[l, dp_me]
        for k in range(n_dp - 1):
            total = total + sq_recv[l, k]
        inverse = lax.rsqrt(total[:, 0:1] / D + epsilon)
        skip_row = v_skip[...].astype(f32)[l : l + 1, :]
        for n in range(CHUNKS):
            settle(part_recv.at[l, n], sem_part.at[l, n, 1])
            summed = part_send[l, n, dp_me].astype(f32)
            for k in range(n_dp - 1):
                summed = summed + part_recv[l, n, k].astype(f32)
            summed = (inverse * summed).astype(bf16).astype(f32)
            drive = summed[:, 0:width]
            gate = summed[:, width:]
            for c in range(tiles):
                tile = n * tiles + c
                g0 = tile * per_tile
                channels = slice(tile * LANES, (tile + 1) * LANES)
                spread = jnp.concatenate(
                    [
                        jnp.where(
                            own_group,
                            jnp.broadcast_to(
                                drive[r : r + 1, c * LANES : (c + 1) * LANES], (per_tile, LANES)
                            ),
                            0.0,
                        )
                        for r in range(own_rows)
                    ],
                    axis=0,
                ).astype(bf16)
                raw = jnp.dot(spread, v_imap[l, channels, :], preferred_element_type=f32)
                a_r, a_i, c_r, c_i = (coef[l, i, g0 : g0 + per_tile, :] for i in range(4))
                history = []
                for s in range(own_seqs):
                    h = v_state[l, s, g0 : g0 + per_tile, :]
                    for t in range(new):
                        r0 = (s * new + t) * per_tile
                        u = raw[r0 : r0 + per_tile]
                        pushed = c_r * u + c_i * pltpu.roll(u, half, 1)
                        after = a_r * h + a_i * pltpu.roll(h, half, 1) + pushed
                        h = jnp.where(t < lens[s], after, h)
                        history.append(h * sign)
                    v_state[l, s, g0 : g0 + per_tile, :] = h
                stacked = jnp.concatenate(history, axis=0).astype(bf16)
                read = lax.dot_general(
                    stacked,
                    v_rmap[l, channels, :],
                    (((1,), (1,)), ((), ())),
                    preferred_element_type=f32,
                )
                for r in range(own_rows):
                    kept = jnp.where(own_group, read[r * per_tile : (r + 1) * per_tile], 0.0)
                    read_rows[r : r + 1, c * LANES : (c + 1) * LANES] = jnp.sum(
                        kept, axis=0, keepdims=True
                    )
            response = read_rows[...] + skip_row[:, n * width : (n + 1) * width] * drive
            branch = jax.nn.gelu(response) * (gate * jax.nn.sigmoid(gate)) * alive
            branch_all[l, n, dp_me] = branch.astype(bf16)
            for peer in dp_peers:
                push(
                    "dp",
                    peer,
                    branch_all.at[l, n, dp_me],
                    branch_all.at[l, n, dp_me],
                    sem_branch.at[l, n],
                )
            sends.append((branch_all.at[l, n, pl.ds(0, n_dp - 1)], sem_branch.at[l, n, 0]))
        saved = local(v_state.at[l], state_out.at[l], sem_out.at[l])

        projected = jnp.zeros((rows, features), f32)
        for n in range(CHUNKS):
            fetch["out", l, n].wait()
            settle(branch_all.at[l, n, pl.ds(0, n_dp - 1)], sem_branch.at[l, n, 1])
            for j in range(n_dp):
                b_rows[j * own_rows : (j + 1) * own_rows, :] = branch_all[l, n, j].astype(f32)
            projected = projected + jnp.dot(
                b_rows[...].astype(bf16), v_out[l, n], preferred_element_type=f32
            )
        if l < layers - 1:
            tp_all[l, tp_me] = projected.astype(bf16)
            for peer in tp_peers:
                push("tp", peer, tp_all.at[l, tp_me], tp_all.at[l, tp_me], sem_tp.at[l])
            sends.append((tp_all.at[l, pl.ds(0, n_tp - 1)], sem_tp.at[l, 0]))
            settle(tp_all.at[l, pl.ds(0, n_tp - 1)], sem_tp.at[l, 1])
            added = tp_all[l, 0].astype(f32)
            for j in range(1, n_tp):
                added = added + tp_all[l, j].astype(f32)
            x = (x + added).astype(bf16).astype(f32)
        else:
            for j in range(n_tp):
                block = slice(j * block_rows, (j + 1) * block_rows)
                rs_send[j] = projected[block].astype(bf16)
                x_recv[j] = x[block].astype(bf16)
            for k, peer in enumerate(tp_peers):
                push("tp", peer, rs_send.at[peer], rs_recv.at[k], sem_rs)
            sends.append((rs_recv, sem_rs.at[0]))
            base = x_recv[tp_me].astype(f32)
            added = rs_send[tp_me].astype(f32)
            settle(rs_recv, sem_rs.at[1])
            for k in range(n_tp - 1):
                added = added + rs_recv[k].astype(f32)
            v_mixed[...] = (base + added).astype(bf16)
            final = local(v_mixed, mixed_out, sem_out.at[layers])
        if l == 0:
            first_saved = [saved]
        else:
            first_saved.append(saved)
        if l == 0:
            settle(*sends.pop(0))
    for ref, sem in sends:
        settle(ref, sem)
    for copy in first_saved:
        copy.wait()
    final.wait()


def body(
    n_tp,
    n_dp,
    tokens,
    lengths,
    norm_gain,
    input_weight,
    gate_weight,
    decay_rate,
    frequency,
    log_step,
    input_map,
    readout_map,
    skip_weight,
    out_weight,
    state,
):
    layers, own_seqs, groups, state_width = state.shape
    block_seqs, new, features = tokens.shape
    inner = input_weight.shape[2]
    width = inner // CHUNKS
    block_rows = block_seqs * new
    rows = lengths.shape[0] * new
    own_rows = own_seqs * new
    any_spec = pl.BlockSpec(memory_space=pl.ANY)
    dma = pltpu.SemaphoreType.DMA
    mixed, new_state = pl.pallas_call(
        functools.partial(kernel, n_tp, n_dp),
        out_shape=(
            jax.ShapeDtypeStruct((block_rows, features), bf16),
            jax.ShapeDtypeStruct(state.shape, f32),
        ),
        in_specs=[pl.BlockSpec(memory_space=pltpu.SMEM)] + [any_spec] * 12,
        out_specs=(any_spec, any_spec),
        scratch_shapes=[
            pltpu.VMEM((layers, features), f32),
            pltpu.VMEM((layers, CHUNKS, features, width), bf16),
            pltpu.VMEM((layers, CHUNKS, features, width), bf16),
            pltpu.VMEM(decay_rate.shape, f32),
            pltpu.VMEM(frequency.shape, f32),
            pltpu.VMEM(log_step.shape, f32),
            pltpu.VMEM((layers, inner, state_width), bf16),
            pltpu.VMEM((layers, inner, state_width), bf16),
            pltpu.VMEM((layers, inner), bf16),
            pltpu.VMEM((layers, CHUNKS, width, features), bf16),
            pltpu.VMEM(state.shape, f32),
            pltpu.VMEM((block_rows, features), bf16),
            pltpu.VMEM((n_tp, block_rows, features), bf16),
            pltpu.VMEM((rows, features), f32),
            pltpu.VMEM((layers, n_dp, own_rows, LANES), f32),
            pltpu.VMEM((layers, n_dp - 1, own_rows, LANES), f32),
            pltpu.VMEM((layers, CHUNKS, n_dp, own_rows, 2 * width), bf16),
            pltpu.VMEM((layers, CHUNKS, n_dp - 1, own_rows, 2 * width), bf16),
            pltpu.VMEM((layers, CHUNKS, n_dp, own_rows, width), bf16),
            pltpu.VMEM((rows, width), f32),
            pltpu.VMEM((own_rows, width), f32),
            pltpu.VMEM((layers, n_tp, rows, features), bf16),
            pltpu.VMEM((n_tp, block_rows, features), bf16),
            pltpu.VMEM((n_tp - 1, block_rows, features), bf16),
            pltpu.VMEM((layers, 4, groups, state_width), f32),
            dma((7,)),
            dma((layers, CHUNKS, 4)),
            dma((layers + 1,)),
            dma((2,)),
            dma((layers, 2)),
            dma((layers, CHUNKS, 2)),
            dma((layers, CHUNKS, 2)),
            dma((layers, 2)),
            dma((2,)),
        ],
        compiler_params=pltpu.CompilerParams(
            collective_id=0, has_side_effects=True, vmem_limit_bytes=60 * 1024 * 1024
        ),
    )(
        lengths,
        tokens.reshape(block_rows, features),
        norm_gain,
        input_weight,
        gate_weight,
        decay_rate,
        frequency,
        log_step,
        input_map.reshape(layers, inner, state_width),
        readout_map.reshape(layers, inner, state_width),
        skip_weight,
        out_weight,
        state,
    )
    return mixed.reshape(tokens.shape), new_state


def solution(mesh):
    return jax.shard_map(
        functools.partial(body, mesh.shape["tp"], mesh.shape["dp"]),
        mesh=mesh,
        in_specs=(
            P(("grp", "tp"), None, "dp"),
            P("grp"),
            P(None, "dp"),
            P(None, "dp", "tp"),
            P(None, "dp", "tp"),
            P(None, "tp", None),
            P(None, "tp", None),
            P(None, "tp"),
            P(None, "tp", None, None),
            P(None, "tp", None, None),
            P(None, "tp"),
            P(None, "tp", "dp"),
            P(None, ("grp", "dp"), "tp", None),
        ),
        out_specs=(P(("grp", "tp"), None, "dp"), P(None, ("grp", "dp"), "tp", None)),
        check_vma=False,
    )
```

```python
import functools

import jax
import jax.numpy as jnp
from jax import lax
from jax.experimental import pallas as pl
from jax.experimental.pallas import tpu as pltpu
from jax.sharding import PartitionSpec as P

D = 4096
S5_IN = 16
CHUNKS = 2
LANES = 128
PLAN = {
    "entry": (("proj", 0),),
    "x0": (("map", 0), ("out", 0)),
    "branch0": (("proj", 1), ("map", 1)),
    "out0": (("out", 1),),
}

epsilon = 1e-06
f32, bf16 = jnp.float32, jnp.bfloat16


def kernel(
    n_tp,
    n_dp,
    lengths,
    tokens,
    norm_gain,
    input_weight,
    gate_weight,
    decay_rate,
    frequency,
    log_step,
    input_map,
    readout_map,
    skip_weight,
    out_weight,
    state,
    mixed_out,
    state_out,
    v_gain,
    v_in,
    v_gate,
    v_decay,
    v_freq,
    v_step,
    v_imap,
    v_rmap,
    v_skip,
    v_out,
    v_state,
    v_mixed,
    x_recv,
    x_all,
    sq_send,
    sq_recv,
    part_send,
    part_recv,
    branch_all,
    b_rows,
    read_rows,
    tp_all,
    rs_send,
    rs_recv,
    coef,
    lens_ref,
    sem_small,
    sem_w,
    sem_out,
    sem_x,
    sem_sq,
    sem_part,
    sem_branch,
    sem_tp,
    sem_rs,
):
    layers, own_seqs, groups, state_width = state.shape
    block_rows, features = tokens.shape
    inner = input_weight.shape[2]
    width = inner // CHUNKS
    all_seqs = lengths.shape[0]
    new = block_rows * n_tp // all_seqs
    own_rows = own_seqs * new
    rows = all_seqs * new
    half = state_width // 2
    per_tile = LANES // S5_IN
    tiles = width // LANES
    tp_me = lax.axis_index("tp")
    dp_me = lax.axis_index("dp")

    def local(src, dst, sem):
        copy = pltpu.make_async_copy(src, dst, sem)
        copy.start()
        return copy

    small = [
        local(src, dst, sem_small.at[i])
        for i, (src, dst) in enumerate(
            (
                (tokens, x_recv.at[tp_me]),
                (norm_gain, v_gain),
                (decay_rate, v_decay),
                (frequency, v_freq),
                (log_step, v_step),
                (skip_weight, v_skip),
                (state, v_state),
                (lengths, lens_ref),
            )
        )
    ]
    fetch = {}

    def load(point):
        for kind, l in PLAN.get(point, ()):
            for n in range(CHUNKS):
                cols = pl.ds(n * width, width)
                if kind == "proj":
                    fetch["in", l, n] = local(
                        input_weight.at[l, :, cols], v_in.at[l, n], sem_w.at[l, n, 0]
                    )
                    fetch["gate", l, n] = local(
                        gate_weight.at[l, :, cols], v_gate.at[l, n], sem_w.at[l, n, 1]
                    )
                elif kind == "out":
                    fetch["out", l, n] = local(
                        out_weight.at[l, cols, :], v_out.at[l, n], sem_w.at[l, n, 2]
                    )
                elif n == 0:
                    fetch["imap", l] = local(input_map.at[l], v_imap.at[l], sem_w.at[l, 0, 3])
                    fetch["rmap", l] = local(readout_map.at[l], v_rmap.at[l], sem_w.at[l, 1, 3])

    load("entry")

    barrier = pltpu.get_barrier_semaphore()
    upper = tp_me // max(n_tp // 2, 1)
    tp_peers = []
    for k in range(n_tp - 1):
        top = n_tp - 1 - k
        low = top - 1 + (top + n_tp - tp_me - 1) // n_tp
        high = k + (k + n_tp - tp_me) // n_tp
        tp_peers.append(low + upper * (high - low))
    dp_peers = [lax.rem(dp_me + k, n_dp) for k in range(1, n_dp)]
    for peer in tp_peers:
        pl.semaphore_signal(
            barrier, inc=1, device_id={"tp": peer}, device_id_type=pl.DeviceIdType.MESH
        )
    for peer in dp_peers:
        pl.semaphore_signal(
            barrier, inc=1, device_id={"dp": peer}, device_id_type=pl.DeviceIdType.MESH
        )
    pl.semaphore_wait(barrier, n_tp + n_dp - 2)

    sends = []
    saves = []

    def push(axis, peer, src, dst, sems):
        copy = pltpu.make_async_remote_copy(
            src_ref=src,
            dst_ref=dst,
            send_sem=sems.at[0],
            recv_sem=sems.at[1],
            device_id={axis: peer},
            device_id_type=pl.DeviceIdType.MESH,
        )
        copy.start()

    def settle(ref, sem):
        pltpu.make_async_copy(ref, ref, sem).wait()

    small[0].wait()
    for peer in tp_peers:
        push("tp", peer, x_recv.at[tp_me], x_recv.at[tp_me], sem_x)
    sends.append((x_recv.at[pl.ds(0, n_tp - 1)], sem_x.at[0]))

    load("sent")
    for copy in small[1:]:
        copy.wait()
    for l in range(layers):
        step = jnp.exp(v_step[l : l + 1, :])
        rate = v_decay[l]
        freq = v_freq[l]
        magnitude = jnp.exp(-rate * step)
        angle = freq * step
        ar = magnitude * jnp.cos(angle)
        ai = magnitude * jnp.sin(angle)
        den = rate * rate + freq * freq
        cr = (-(ar - 1.0) * rate + ai * freq) / den
        ci = (-ai * rate - (ar - 1.0) * freq) / den
        for i, (low, high) in enumerate(((ar, ar), (-ai, ai), (cr, cr), (-ci, ci))):
            coef[l, i] = jnp.concatenate([low, high], axis=0).T

    settle(x_recv.at[pl.ds(0, n_tp - 1)], sem_x.at[1])
    for j in range(n_tp):
        x_all[j * block_rows : (j + 1) * block_rows, :] = x_recv[j].astype(f32)
    x = x_all[...]
    load("x0")

    lane = lax.broadcasted_iota(jnp.int32, (per_tile, LANES), 1)
    sub = lax.broadcasted_iota(jnp.int32, (per_tile, LANES), 0)
    own_group = (lane >= sub * S5_IN) & (lane < (sub + 1) * S5_IN)
    sign = jnp.where(
        lax.broadcasted_iota(jnp.int32, (1, state_width), 1) < half, jnp.float32(1), jnp.float32(-1)
    )
    lens = [lens_ref[dp_me * own_seqs + s] for s in range(own_seqs)]
    row_id = lax.broadcasted_iota(jnp.int32, (own_rows, 1), 0)
    alive = jnp.zeros((own_rows, 1), f32)
    for s in range(own_seqs):
        inside = (row_id >= s * new) & (row_id < s * new + lens[s])
        alive = jnp.where(inside, jnp.float32(1), alive)

    for l in range(layers):
        squares = jnp.sum(x * x, axis=1, keepdims=True)
        wide = jnp.broadcast_to(squares, (rows, LANES))
        for j in range(n_dp):
            sq_send[l, j] = wide[j * own_rows : (j + 1) * own_rows, :]
        for k, peer in enumerate(dp_peers):
            push("dp", peer, sq_send.at[l, peer], sq_recv.at[l, k], sem_sq.at[l])
        sends.append((sq_recv.at[l], sem_sq.at[l, 0]))
        scaled = (x * v_gain[l : l + 1, :]).astype(bf16)
        for n in range(CHUNKS):
            fetch["in", l, n].wait()
            drive_part = jnp.dot(scaled, v_in[l, n], preferred_element_type=f32)
            fetch["gate", l, n].wait()
            gate_part = jnp.dot(scaled, v_gate[l, n], preferred_element_type=f32)
            for j in range(n_dp):
                own = slice(j * own_rows, (j + 1) * own_rows)
                part_send[l, n, j, :, 0:width] = drive_part[own].astype(bf16)
                part_send[l, n, j, :, width:] = gate_part[own].astype(bf16)
            for k, peer in enumerate(dp_peers):
                push("dp", peer, part_send.at[l, n, peer], part_recv.at[l, n, k], sem_part.at[l, n])
            sends.append((part_recv.at[l, n], sem_part.at[l, n, 0]))

        load(f"proj{l}")
        fetch["imap", l].wait()
        fetch["rmap", l].wait()
        settle(sq_recv.at[l], sem_sq.at[l, 1])
        total = sq_send[l, dp_me]
        for k in range(n_dp - 1):
            total = total + sq_recv[l, k]
        inverse = lax.rsqrt(total[:, 0:1] / D + epsilon)
        skip_row = v_skip[...].astype(f32)[l : l + 1, :]
        for n in range(CHUNKS):
            settle(part_recv.at[l, n], sem_part.at[l, n, 1])
            summed = part_send[l, n, dp_me].astype(f32)
            for k in range(n_dp - 1):
                summed = summed + part_recv[l, n, k].astype(f32)
            summed = (inverse * summed).astype(bf16).astype(f32)
            drive = summed[:, 0:width]
            gate = summed[:, width:]
            pieces = []
            for c in range(tiles):
                for r in range(own_rows):
                    spread = jnp.broadcast_to(
                        drive[r : r + 1, c * LANES : (c + 1) * LANES], (per_tile, LANES)
                    )
                    pieces.append(jnp.where(own_group, spread, 0.0))
            raws = []
            for c in range(tiles):
                tile = n * tiles + c
                spread = jnp.concatenate(pieces[c * own_rows : (c + 1) * own_rows], axis=0)
                raws.append(
                    jnp.dot(
                        spread.astype(bf16),
                        v_imap[l, tile * LANES : (tile + 1) * LANES, :],
                        preferred_element_type=f32,
                    )
                )
            here = slice(n * tiles * per_tile, (n + 1) * tiles * per_tile)
            a_r, a_i, c_r, c_i = (coef[l, i, here, :] for i in range(4))
            history = []
            for s in range(own_seqs):
                h = v_state[l, s, here, :]
                for t in range(new):
                    r0 = (s * new + t) * per_tile
                    u = jnp.concatenate([raw[r0 : r0 + per_tile] for raw in raws], axis=0)
                    pushed = c_r * u + c_i * pltpu.roll(u, half, 1)
                    after = a_r * h + a_i * pltpu.roll(h, half, 1) + pushed
                    h = jnp.where(t < lens[s], after, h)
                    history.append((h * sign).astype(f32))
                state_out[l, s, here, :] = h
            reads = []
            for c in range(tiles):
                tile = n * tiles + c
                stacked = jnp.concatenate(
                    [h[c * per_tile : (c + 1) * per_tile] for h in history], axis=0
                ).astype(bf16)
                reads.append(
                    lax.dot_general(
                        stacked,
                        v_rmap[l, tile * LANES : (tile + 1) * LANES, :],
                        (((1,), (1,)), ((), ())),
                        preferred_element_type=f32,
                    )
                )
            for c in range(tiles):
                for r in range(own_rows):
                    kept = jnp.where(own_group, reads[c][r * per_tile : (r + 1) * per_tile], 0.0)
                    read_rows[r : r + 1, c * LANES : (c + 1) * LANES] = jnp.sum(
                        kept, axis=0, keepdims=True
                    )
            response = read_rows[...] + skip_row[:, n * width : (n + 1) * width] * drive
            branch = jax.nn.gelu(response) * (gate * jax.nn.sigmoid(gate)) * alive
            branch_all[l, n, dp_me] = branch.astype(bf16)
            for peer in dp_peers:
                push(
                    "dp",
                    peer,
                    branch_all.at[l, n, dp_me],
                    branch_all.at[l, n, dp_me],
                    sem_branch.at[l, n],
                )
            sends.append((branch_all.at[l, n, pl.ds(0, n_dp - 1)], sem_branch.at[l, n, 0]))
        load(f"branch{l}")

        projected = jnp.zeros((rows, features), f32)
        for n in range(CHUNKS):
            fetch["out", l, n].wait()
            settle(branch_all.at[l, n, pl.ds(0, n_dp - 1)], sem_branch.at[l, n, 1])
            for j in range(n_dp):
                b_rows[j * own_rows : (j + 1) * own_rows, :] = branch_all[l, n, j].astype(f32)
            projected = projected + jnp.dot(
                b_rows[...].astype(bf16), v_out[l, n], preferred_element_type=f32
            )
        if l < layers - 1:
            tp_all[l, tp_me] = projected.astype(bf16)
            for peer in tp_peers:
                push("tp", peer, tp_all.at[l, tp_me], tp_all.at[l, tp_me], sem_tp.at[l])
            sends.append((tp_all.at[l, pl.ds(0, n_tp - 1)], sem_tp.at[l, 0]))
            load(f"out{l}")
            settle(tp_all.at[l, pl.ds(0, n_tp - 1)], sem_tp.at[l, 1])
            added = tp_all[l, 0].astype(f32)
            for j in range(1, n_tp):
                added = added + tp_all[l, j].astype(f32)
            x = (x + added).astype(bf16).astype(f32)
        else:
            for j in range(n_tp):
                block = slice(j * block_rows, (j + 1) * block_rows)
                rs_send[j] = projected[block].astype(bf16)
                x_recv[j] = x[block].astype(bf16)
            for peer in tp_peers:
                slot = lax.rem(tp_me - peer + n_tp, n_tp) - 1
                push("tp", peer, rs_send.at[peer], rs_recv.at[slot], sem_rs)
            for ref, sem in sends:
                settle(ref, sem)
            for copy in saves:
                copy.wait()
            base = x_recv[tp_me].astype(f32)
            added = rs_send[tp_me].astype(f32)
            settle(rs_recv, sem_rs.at[1])
            for k in range(n_tp - 1):
                added = added + rs_recv[k].astype(f32)
            mixed_out[...] = (base + added).astype(bf16)
        if l == 0:
            settle(*sends.pop(0))
    settle(rs_recv, sem_rs.at[0])


def body(
    n_tp,
    n_dp,
    tokens,
    lengths,
    norm_gain,
    input_weight,
    gate_weight,
    decay_rate,
    frequency,
    log_step,
    input_map,
    readout_map,
    skip_weight,
    out_weight,
    state,
):
    layers, own_seqs, groups, state_width = state.shape
    block_seqs, new, features = tokens.shape
    inner = input_weight.shape[2]
    width = inner // CHUNKS
    block_rows = block_seqs * new
    rows = lengths.shape[0] * new
    own_rows = own_seqs * new
    any_spec = pl.BlockSpec(memory_space=pl.ANY)
    dma = pltpu.SemaphoreType.DMA
    mixed, new_state = pl.pallas_call(
        functools.partial(kernel, n_tp, n_dp),
        out_shape=(
            pltpu.VMEM((block_rows, features), bf16),
            pltpu.VMEM(state.shape, f32),
        ),
        in_specs=[any_spec] * 13,
        out_specs=(pl.BlockSpec(memory_space=pltpu.VMEM),) * 2,
        scratch_shapes=[
            pltpu.VMEM((layers, features), f32),
            pltpu.VMEM((layers, CHUNKS, features, width), bf16),
            pltpu.VMEM((layers, CHUNKS, features, width), bf16),
            pltpu.VMEM((layers, state_width // 2, groups), f32),
            pltpu.VMEM((layers, state_width // 2, groups), f32),
            pltpu.VMEM(log_step.shape, f32),
            pltpu.VMEM((layers, inner, state_width), bf16),
            pltpu.VMEM((layers, inner, state_width), bf16),
            pltpu.VMEM((layers, inner), bf16),
            pltpu.VMEM((layers, CHUNKS, width, features), bf16),
            pltpu.VMEM(state.shape, f32),
            pltpu.VMEM((block_rows, features), bf16),
            pltpu.VMEM((n_tp, block_rows, features), bf16),
            pltpu.VMEM((rows, features), f32),
            pltpu.VMEM((layers, n_dp, own_rows, LANES), f32),
            pltpu.VMEM((layers, n_dp - 1, own_rows, LANES), f32),
            pltpu.VMEM((layers, CHUNKS, n_dp, own_rows, 2 * width), bf16),
            pltpu.VMEM((layers, CHUNKS, n_dp - 1, own_rows, 2 * width), bf16),
            pltpu.VMEM((layers, CHUNKS, n_dp, own_rows, width), bf16),
            pltpu.VMEM((rows, width), f32),
            pltpu.VMEM((own_rows, width), f32),
            pltpu.VMEM((layers, n_tp, rows, features), bf16),
            pltpu.VMEM((n_tp, block_rows, features), bf16),
            pltpu.VMEM((n_tp - 1, block_rows, features), bf16),
            pltpu.VMEM((layers, 4, groups, state_width), f32),
            pltpu.SMEM(lengths.shape, jnp.int32),
            dma((8,)),
            dma((layers, CHUNKS, 4)),
            dma((layers + 1,)),
            dma((2,)),
            dma((layers, 2)),
            dma((layers, CHUNKS, 2)),
            dma((layers, CHUNKS, 2)),
            dma((layers, 2)),
            dma((2,)),
        ],
        compiler_params=pltpu.CompilerParams(
            collective_id=0, has_side_effects=True, vmem_limit_bytes=60 * 1024 * 1024
        ),
    )(
        lengths,
        tokens.reshape(block_rows, features),
        norm_gain,
        input_weight,
        gate_weight,
        jnp.swapaxes(decay_rate, 1, 2),
        jnp.swapaxes(frequency, 1, 2),
        log_step,
        input_map.reshape(layers, inner, state_width),
        readout_map.reshape(layers, inner, state_width),
        skip_weight,
        out_weight,
        state,
    )
    return mixed.reshape(tokens.shape), new_state


def solution(mesh):
    return jax.shard_map(
        functools.partial(body, mesh.shape["tp"], mesh.shape["dp"]),
        mesh=mesh,
        in_specs=(
            P(("grp", "tp"), None, "dp"),
            P("grp"),
            P(None, "dp"),
            P(None, "dp", "tp"),
            P(None, "dp", "tp"),
            P(None, "tp", None),
            P(None, "tp", None),
            P(None, "tp"),
            P(None, "tp", None, None),
            P(None, "tp", None, None),
            P(None, "tp"),
            P(None, "tp", "dp"),
            P(None, ("grp", "dp"), "tp", None),
        ),
        out_specs=(P(("grp", "tp"), None, "dp"), P(None, ("grp", "dp"), "tp", None)),
        check_vma=False,
    )
```
